32 devices in a mesh: grp: 2 (over y), fs: 4 (over z), tp: 4 (over x, core).
Axes of the slice: x: 2, y: 2, z: 4, core: 2. Of those that a mesh axis runs over, the one named last changes fastest.
Arguments:
- tokens: bfloat16 [2048, 2048], P(('grp', 'fs'), 'tp'), parts along dimension 0, may hold values from -6 to 6
- route_experts: int32 [2048, 2], P(('grp', 'fs')), parts along dimension 0, may hold values from 0 to 15, as said below
- group_weight: float32 [2048], P(('grp', 'fs')), parts along dimension 0, may hold values from 0.2 to 1
- pair_logit: float32 [2048], P(('grp', 'fs')), parts along dimension 0, may hold values from -6 to 6
- norm_gain: float32 [2048], replicated, may hold values from 0.1 to 1.9
- gate_train: float32 [16, 2048, 2048], P(None, 'fs', 'tp'), may hold values from -0.125 to 0.125
- up_train: float32 [16, 2048, 2048], P(None, 'fs', 'tp'), may hold values from -0.125 to 0.125
- down_train: float32 [16, 2048, 2048], P(None, 'fs', 'tp'), may hold values from -0.125 to 0.125
Outputs:
- gate_serve: bfloat16 [32, 2048, 2048], P(('grp', 'fs'), None, 'tp'), parts along dimension 0
- up_serve: bfloat16 [32, 2048, 2048], P(('grp', 'fs'), None, 'tp'), parts along dimension 0
- down_serve: bfloat16 [32, 2048, 2048], P(('grp', 'fs'), None, 'tp'), parts along dimension 0
- moe_out: bfloat16 [2048, 2048], P(('grp', 'fs'), 'tp'), parts along dimension 0
The draws below stay inside these ranges and needn't reach their ends.
There are 2 independent parts, one for each index of `grp`. The reference program is written for one: setup_inputs(seed, part) draws one part's arguments, and reference() takes and returns one part's arrays. A program takes and returns all parts, laid end to end along the dimension named above; an argument that names none is the same for every part. Nothing has to cross between parts.
Inputs may be any that keep to these rules, and one draw needn't show every extreme that they name: `route_experts`: each row names two different experts of the same group of 4 consecutive expert numbers. Among the 256 aligned rows of one index of fs, no expert is named by more than 64 rows, and in every draw some expert is named by exactly 64 rows from every such block.
All inputs are finite; a program needn't handle non-finite values.
Results may differ from the reference program's by a relative error of at most 0.018.
Values may be sent and summed in bfloat16 or wider, within the bound.
No kernel may reach another device: no remote copies, remote signals or barrier semaphores. Data moves between devices by JAX's collectives and lax.ppermute only.
A program may use at most 192 MiB of HBM per device.

```python
import math
import jax
import jax.numpy as jnp
from jax import lax

D = 2048
FF = 2048
GROUPS = 4
PER_GROUP = 4
TOK_DEV = 256
EXPERTS = 16
CAP = 64
TOKENS = 1024
N_FS = 4
N_TP = 4


def draw_route_experts(key, part):
    blocks = TOKENS // TOK_DEV
    busiest = jax.random.randint(jax.random.fold_in(key, 7), (), 0, GROUPS)
    block_keys = jax.random.split(jax.random.fold_in(key, 11), blocks)
    group_ids = jnp.arange(GROUPS, dtype=jnp.int32)

    def one_block(block_key):
        cut_key, relabel_key, shuffle_key = jax.random.split(block_key, 3)
        remainder = TOK_DEV - 2 * CAP
        cut_points = jnp.sort(jax.random.randint(cut_key, (2,), 0, remainder + 1))
        others = jnp.stack([cut_points[0], cut_points[1] - cut_points[0], remainder - cut_points[1]])
        other_slot = jnp.minimum((group_ids - busiest - 1) % GROUPS, 2)
        counts = jnp.where(group_ids == busiest, 2 * CAP, others[other_slot])
        group_ends = jnp.cumsum(counts)
        group_starts = group_ends - counts
        positions = jnp.arange(TOK_DEV, dtype=jnp.int32)
        member = jnp.sum((positions[:, None] >= group_ends[None, :]).astype(jnp.int32), axis=1)
        member = jnp.minimum(member, GROUPS - 1)
        within = positions - group_starts[member]
        first_rank = within % PER_GROUP
        second = (first_rank + 1 + within // PER_GROUP % (PER_GROUP - 1)) % PER_GROUP

        def relabel_group(group):
            return jax.random.permutation(jax.random.fold_in(relabel_key, group), PER_GROUP)
        relabel = jax.vmap(relabel_group)(group_ids)
        chosen_pair = jnp.stack([member * PER_GROUP + relabel[member, first_rank], member * PER_GROUP + relabel[member, second]], axis=1)
        shuffle = jax.random.permutation(shuffle_key, TOK_DEV)
        return chosen_pair[shuffle]
    return jax.vmap(one_block)(block_keys).reshape(TOKENS, 2).astype(jnp.int32)


def shard_levels(key, shape, pieces, smallest, high):
    loudness = 1.0
    for position, blocks in pieces:
        draws = jax.random.uniform(jax.random.fold_in(jax.random.fold_in(key, 6), position), (blocks,), jnp.float32, smallest / len(pieces), high / len(pieces))
        loudness = loudness * jnp.repeat(jnp.exp(draws), shape[position] // blocks).reshape((-1,) + (1,) * (len(shape) - 1 - position))
    return loudness


def normal_values(own_key, shape, width, most, shards=(), kind=jnp.bfloat16):
    values = width * jax.random.normal(own_key, shape, jnp.float32)
    if shards:
        values = values * shard_levels(own_key, shape, shards, -0.22, 0.18)
    return jnp.clip(values, -most, most).astype(kind)


def setup_inputs(seed: int = 0, part: int = 0) -> dict:
    streams_of = jax.random.split(jax.random.key(seed), 9)
    own_keys = jax.random.split(jax.random.fold_in(streams_of[8], part), 9)
    return {
        "tokens": normal_values(own_keys[0], (TOKENS, D), 1.0, 6.0, ((0, 4), (1, 4))),
        "route_experts": draw_route_experts(jax.random.fold_in(jax.random.fold_in(streams_of[8], part), 71), part),
        "group_weight": jnp.clip(jnp.exp(math.log(1.0) - 1.609438 * jax.random.uniform(own_keys[2], (TOKENS,), jnp.float32) ** shard_levels(own_keys[2], (TOKENS,), ((0, 4),), -0.2, 0.2)), 0.2, 1.0),
        "pair_logit": normal_values(own_keys[3], (TOKENS,), 1.5, 6.0, ((0, 4),), jnp.float32),
        "norm_gain": jnp.clip(1.0 + 0.18 * jax.random.normal(streams_of[4], (D,), jnp.float32), 0.1, 1.9),
        "gate_train": normal_values(streams_of[5], (EXPERTS, D, FF), D ** -0.5, 0.125, ((1, 4), (2, 4)), jnp.float32),
        "up_train": normal_values(streams_of[6], (EXPERTS, D, FF), D ** -0.5, 0.125, ((1, 4), (2, 4)), jnp.float32),
        "down_train": normal_values(streams_of[7], (EXPERTS, D, FF), FF ** -0.5, 0.125, ((1, 4), (2, 4)), jnp.float32),
    }


def reference(tokens, route_experts, group_weight, pair_logit, norm_gain, gate_train, up_train, down_train):
    gate_serve = (norm_gain[None, :, None] * gate_train).astype(jnp.bfloat16)
    up_serve = (norm_gain[None, :, None] * up_train).astype(jnp.bfloat16)
    down_serve = down_train.astype(jnp.bfloat16)
    as_float = tokens.astype(jnp.float32)
    row_scale = lax.rsqrt(lax.optimization_barrier(jnp.mean(as_float * as_float, axis=1)) + 1e-06)
    first_gate = group_weight * jax.nn.sigmoid(pair_logit)
    second_gate = group_weight * jax.nn.sigmoid(-pair_logit)
    most_rows = N_FS * CAP
    block_width = FF // N_TP

    def add_expert(expert, running):
        first_hit = route_experts[:, 0] == expert
        second_hit = route_experts[:, 1] == expert
        row_weight = jnp.where(first_hit, first_gate, 0.0) + jnp.where(second_hit, second_gate, 0.0)
        sort_key = jnp.where(first_hit | second_hit, 0, 1).astype(jnp.int32)
        row_order = jnp.argsort(sort_key, stable=True)[:most_rows].astype(jnp.int32)
        picked = tokens[row_order]
        picked_scale = row_scale[row_order][:, None]
        gate_pre = picked_scale * jnp.dot(picked, gate_serve[expert], preferred_element_type=jnp.float32)
        up_pre = picked_scale * jnp.dot(picked, up_serve[expert], preferred_element_type=jnp.float32)
        hidden = (jax.nn.silu(gate_pre) * up_pre).astype(jnp.bfloat16)
        down_expert = down_serve[expert]

        def add_block(block, partial_sum):
            column = (block * block_width).astype(jnp.int32)
            hidden_part = lax.dynamic_slice_in_dim(hidden, column, block_width, 1)
            down_part = lax.dynamic_slice_in_dim(down_expert, column, block_width, 1)
            partial_value = jnp.dot(hidden_part, down_part.T, preferred_element_type=jnp.float32).astype(jnp.bfloat16)
            partial_value = lax.optimization_barrier(partial_value)
            return partial_sum + partial_value.astype(jnp.float32)
        summed = lax.fori_loop(0, N_TP, add_block, jnp.zeros((most_rows, D), jnp.float32))
        routed = lax.optimization_barrier(summed.astype(jnp.bfloat16)).astype(jnp.float32)
        return running.at[row_order].add(row_weight[row_order][:, None] * routed)
    total = lax.fori_loop(0, EXPERTS, add_expert, jnp.zeros((TOKENS, D), jnp.float32))
    return (gate_serve, up_serve, down_serve, total.astype(jnp.bfloat16))
```

```python
import jax
import jax.numpy as jnp
from jax import lax
from jax.sharding import PartitionSpec as P

CAP = 64
GROUP = 4
DOWN_CHUNKS = 2


def target(i, m, n):
    return i ^ m if n & (n - 1) == 0 else (i + m) % n


def origin(i, m, n):
    return i ^ m if n & (n - 1) == 0 else (i - m) % n


def hop(x, axis, m):
    n = lax.axis_size(axis)
    return lax.ppermute(x, axis, [(i, target(i, m, n)) for i in range(n)])


def hop_back(x, axis, m):
    n = lax.axis_size(axis)
    return lax.ppermute(x, axis, [(target(i, m, n), i) for i in range(n)])


def shards(
    tokens, route_experts, group_weight, pair_logit, norm_gain, gate_train, up_train, down_train
):
    bf16, f32 = jnp.bfloat16, jnp.float32
    experts, rows_here, hidden_here = gate_train.shape
    model_width = norm_gain.shape[0]
    tok_rows, feats = tokens.shape
    owners, copies, splits = lax.axis_size("fs"), lax.axis_size("grp"), lax.axis_size("tp")
    here, copy, split = lax.axis_index("fs"), lax.axis_index("grp"), lax.axis_index("tp")
    per_owner = experts // owners
    chunks = DOWN_CHUNKS if owners == splits else 1

    gain_rows = lax.dynamic_slice_in_dim(norm_gain, here * rows_here, rows_here)

    def scaled(train, gain, parts, owner, part, share):
        rows = rows_here // (parts * copies)
        view = train.reshape(owners, per_owner, parts, copies, rows, hidden_here)
        block = lax.dynamic_slice(
            view, (owner, 0, part, share, 0, 0), (1, per_owner, 1, 1, rows, hidden_here)
        ).reshape(per_owner, rows, hidden_here)
        if gain is None:
            return block.astype(bf16)
        gain_view = gain.reshape(parts, copies, rows)
        gain_block = lax.dynamic_slice(gain_view, (part, share, 0), (1, 1, rows)).reshape(rows)
        return (gain_block[None, :, None] * block).astype(bf16)

    def send(train, gain, parts, part):
        return [
            hop(scaled(train, gain, parts, target(here, m, owners), part, copy), "fs", m)
            for m in range(1, owners)
        ]

    def start(train, gain, parts):
        rows = rows_here // (parts * copies)
        serve = jnp.zeros((per_owner, owners, parts, copies, rows, hidden_here), bf16)
        view = train.reshape(owners, per_owner, parts, copies, rows, hidden_here)
        block = lax.dynamic_slice(
            view, (here, 0, 0, 0, 0, 0), (1,) + view.shape[1:]
        ).reshape((per_owner, 1) + view.shape[2:])
        if gain is not None:
            block = gain.reshape(1, 1, parts, copies, rows, 1) * block
        return lax.dynamic_update_slice(serve, block.astype(bf16), (0, here, 0, 0, 0, 0))

    def place(serve, pieces, part):
        for m, piece in zip(range(1, owners), pieces):
            source = origin(here, m, owners)
            shape = (per_owner, 1, 1, 1) + piece.shape[1:]
            others = [(origin(copy, k, copies), hop(piece, "grp", k)) for k in range(1, copies)]
            for share, block in [(copy, piece)] + others:
                serve = lax.dynamic_update_slice(
                    serve, block.reshape(shape), (0, source, part, share, 0, 0)
                )
        return serve

    gate_pieces = send(gate_train, gain_rows, 1, 0)

    paired = per_owner % GROUP == 0
    slots = per_owner * CAP // 2 if paired else per_owner * CAP
    if paired:
        owner_of = route_experts[:, :1] // per_owner
        cells = jnp.arange(owners, dtype=jnp.int32)
    else:
        owner_of = route_experts
        cells = jnp.arange(experts, dtype=jnp.int32)
    picks = owner_of.shape[1]
    flat = owner_of.reshape(tok_rows * picks)
    hits = (flat[:, None] == cells[None, :]).astype(f32)
    items = jnp.arange(tok_rows * picks, dtype=jnp.int32)
    earlier = (items[None, :] < items[:, None]).astype(f32)
    before = jnp.dot(earlier, hits, preferred_element_type=f32)
    rank = jnp.sum(before * hits, axis=1).astype(jnp.int32)
    size = slots * owners // cells.shape[0]
    slot_of = (rank + size * flat).reshape(tok_rows, picks)
    order = jnp.stack([target(here, m, owners) for m in range(owners)])
    slot_ids = (order[:, None] * slots + jnp.arange(slots, dtype=jnp.int32)[None, :]).reshape(-1)
    placed = [slot_of[:, k : k + 1] == slot_ids[None, :] for k in range(picks)]
    pick_rows = (placed[0] | placed[-1]).astype(bf16)
    gates = (
        group_weight * jax.nn.sigmoid(pair_logit),
        group_weight * jax.nn.sigmoid(-pair_logit),
    )
    local_ids = jnp.arange(per_owner, dtype=jnp.int32)
    weights = 0.0
    for k in range(2):
        local = jnp.where(
            (route_experts[:, k] % per_owner)[:, None] == local_ids[None, :], gates[k][:, None], 0.0
        )
        weights = weights + lax.dot_general(
            local,
            placed[min(k, picks - 1)].astype(f32),
            (((0,), (0,)), ((), ())),
            precision=lax.Precision.HIGHEST,
            preferred_element_type=f32,
        )
    outgoing = lax.dot_general(
        pick_rows, tokens, (((0,), (0,)), ((), ())), preferred_element_type=f32
    ).astype(bf16)
    arrived = [outgoing[:slots]]
    arrived_weights = [weights[:, :slots]]
    for m in range(1, owners):
        arrived.append(hop(outgoing[m * slots : (m + 1) * slots], "fs", m))
        arrived_weights.append(hop(weights[:, m * slots : (m + 1) * slots], "fs", m))
    rows = jnp.concatenate(arrived, axis=0)
    row_weights = jnp.concatenate(arrived_weights, axis=1)

    up_pieces = send(up_train, gain_rows, 1, 0)
    down_pieces = [send(down_train, None, chunks, q) for q in range(chunks)]

    slots_all = owners * slots
    section = jnp.zeros((splits, slots_all, feats), bf16)
    for m in range(splits):
        block = hop(rows, "tp", m) if m else rows
        section = lax.dynamic_update_slice(
            section, block[None], (origin(split, m, splits), 0, 0)
        )
    squares = jnp.sum(jnp.square(section.astype(f32)), axis=(0, 2))
    row_scale = lax.rsqrt(squares / model_width + 1e-06)
    section = jnp.transpose(section, (1, 0, 2)).reshape(slots_all, model_width)

    serve_shape = (per_owner, model_width, hidden_here)
    gate_serve = place(start(gate_train, gain_rows, 1), gate_pieces, 0).reshape(serve_shape)
    gate_pre = row_scale[None, :, None] * jnp.einsum(
        "rk,ekf->erf", section, gate_serve, preferred_element_type=f32
    )
    gate_act = row_weights[:, :, None] * jax.nn.silu(gate_pre)
    up_serve = place(start(up_train, gain_rows, 1), up_pieces, 0).reshape(serve_shape)
    up_pre = row_scale[None, :, None] * jnp.einsum(
        "rk,ekf->erf", section, up_serve, preferred_element_type=f32
    )
    hidden = (gate_act * up_pre).astype(bf16)

    down_serve = start(down_train, None, chunks)
    outs = []
    for q in range(chunks):
        down_serve = place(down_serve, down_pieces[q], q)
        part = down_serve[:, :, q]
        part = part.reshape(per_owner, splits, -1, hidden_here)
        partial = jnp.einsum("erf,etdf->trd", hidden, part, preferred_element_type=f32)
        partial = partial.astype(bf16)
        if q + 1 < chunks:
            down_serve, partial = lax.optimization_barrier((down_serve, partial))
        total = 0.0
        for m in range(splits):
            block = lax.dynamic_index_in_dim(partial, target(split, m, splits), 0, False)
            block = hop(block, "tp", m) if m else block
            total = total + block.astype(f32)
        total = total.astype(bf16)
        back = [total[:slots]]
        for m in range(1, owners):
            back.append(hop_back(total[m * slots : (m + 1) * slots], "fs", m))
        back = jnp.concatenate(back, axis=0)
        outs.append(jnp.dot(pick_rows, back, preferred_element_type=f32).astype(bf16))
    moe_out = jnp.concatenate(outs, axis=1)
    return gate_serve, up_serve, down_serve.reshape(serve_shape), moe_out


def solution(mesh):
    in_specs = (
        P(("grp", "fs"), "tp"),
        P(("grp", "fs"), None),
        P(("grp", "fs")),
        P(("grp", "fs")),
        P(),
        P(None, "fs", "tp"),
        P(None, "fs", "tp"),
        P(None, "fs", "tp"),
    )
    out_specs = (
        P(("grp", "fs"), None, "tp"),
        P(("grp", "fs"), None, "tp"),
        P(("grp", "fs"), None, "tp"),
        P(("grp", "fs"), "tp"),
    )
    return jax.shard_map(shards, mesh=mesh, in_specs=in_specs, out_specs=out_specs, check_vma=False)
```

```python
import jax
import jax.numpy as jnp
from jax import lax
from jax.sharding import PartitionSpec as P

CAP = 64
GROUP = 4
DOWN_PARTS = (2, 1, 1)


def target(i, m, n):
    return i ^ m if n & (n - 1) == 0 else (i + m) % n


def origin(i, m, n):
    return i ^ m if n & (n - 1) == 0 else (i - m) % n


def distance(i, source, n):
    return i ^ source if n & (n - 1) == 0 else (i - source) % n


def hop(x, axis, m):
    n = lax.axis_size(axis)
    return lax.ppermute(x, axis, [(i, target(i, m, n)) for i in range(n)])


def hop_back(x, axis, m):
    n = lax.axis_size(axis)
    return lax.ppermute(x, axis, [(target(i, m, n), i) for i in range(n)])


def shards(
    tokens, route_experts, group_weight, pair_logit, norm_gain, gate_train, up_train, down_train
):
    bf16, f32 = jnp.bfloat16, jnp.float32
    experts, rows_here, hidden_here = gate_train.shape
    model_width = norm_gain.shape[0]
    tok_rows, feats = tokens.shape
    owners, copies, splits = lax.axis_size("fs"), lax.axis_size("grp"), lax.axis_size("tp")
    here, copy, split = lax.axis_index("fs"), lax.axis_index("grp"), lax.axis_index("tp")
    per_owner = experts // owners
    parts = DOWN_PARTS if owners == splits else (1,)
    unit = rows_here // (copies * sum(parts))
    sizes = [part * unit for part in parts]
    firsts = [unit * sum(parts[:i]) for i in range(len(parts))]

    gain_rows = lax.dynamic_slice_in_dim(norm_gain, here * rows_here, rows_here)
    share_rows = rows_here // copies
    gain_view = gain_rows.reshape(copies, share_rows)
    view_shape = (owners, per_owner, copies, share_rows, hidden_here)

    def cast(train, gain, owner, share, first, rows):
        block = lax.dynamic_slice(
            train.reshape(view_shape),
            (owner, 0, share, first, 0),
            (1, per_owner, 1, rows, hidden_here),
        ).reshape(per_owner, rows, hidden_here)
        if gain:
            scale = lax.dynamic_slice(gain_view, (share, first), (1, rows))
            block = scale.reshape(1, rows, 1) * block
        return block.astype(bf16)

    def send(train, gain, first, rows, after):
        pieces = []
        for m in range(1, owners):
            at, _ = lax.optimization_barrier((here, after))
            after = cast(train, gain, target(at, m, owners), copy, first, rows)
            pieces.append(hop(after, "fs", m))
        return pieces, after

    def swap(piece):
        return [hop(piece, "grp", k) for k in range(1, copies)]

    def own(train, gain, first, rows):
        return [cast(train, gain, here, origin(copy, k, copies), first, rows) for k in range(copies)]

    def begin():
        return jnp.zeros((per_owner, owners, copies, share_rows, hidden_here), bf16)

    def place(serve, m, blocks, first):
        for k, block in enumerate(blocks):
            shape = (per_owner, 1, 1) + block.shape[1:]
            spot = (0, origin(here, m, owners), origin(copy, k, copies), first, 0)
            serve = lax.dynamic_update_slice(serve, block.reshape(shape), spot)
        return serve

    gate_pieces, after = send(gate_train, True, 0, share_rows, norm_gain)

    paired = per_owner % GROUP == 0
    slots = per_owner * CAP // 2 if paired else per_owner * CAP
    if paired:
        owner_of = route_experts[:, :1] // per_owner
        cells = jnp.arange(owners, dtype=jnp.int32)
    else:
        owner_of = route_experts
        cells = jnp.arange(experts, dtype=jnp.int32)
    picks = owner_of.shape[1]
    flat = owner_of.reshape(tok_rows * picks)
    hits = (flat[:, None] == cells[None, :]).astype(f32)
    items = jnp.arange(tok_rows * picks, dtype=jnp.int32)
    earlier = (items[None, :] < items[:, None]).astype(f32)
    before = jnp.dot(earlier, hits, preferred_element_type=f32)
    rank = jnp.sum(before * hits, axis=1).astype(jnp.int32)
    size = slots * owners // cells.shape[0]
    slot_of = (rank + size * flat).reshape(tok_rows, picks)
    order = jnp.stack([target(here, m, owners) for m in range(owners)])
    slot_ids = (order[:, None] * slots + jnp.arange(slots, dtype=jnp.int32)[None, :]).reshape(-1)
    placed = [slot_of[:, k : k + 1] == slot_ids[None, :] for k in range(picks)]
    pick_rows = (placed[0] | placed[-1]).astype(bf16)
    gates = (
        group_weight * jax.nn.sigmoid(pair_logit),
        group_weight * jax.nn.sigmoid(-pair_logit),
    )
    local_ids = jnp.arange(per_owner, dtype=jnp.int32)
    weights = 0.0
    for k in range(2):
        local = jnp.where(
            (route_experts[:, k] % per_owner)[:, None] == local_ids[None, :], gates[k][:, None], 0.0
        )
        weights = weights + lax.dot_general(
            local,
            placed[min(k, picks - 1)].astype(f32),
            (((0,), (0,)), ((), ())),
            precision=lax.Precision.HIGHEST,
            preferred_element_type=f32,
        )
    outgoing = lax.dot_general(
        pick_rows, tokens, (((0,), (0,)), ((), ())), preferred_element_type=f32
    ).astype(bf16)
    arrived = [outgoing[:slots]]
    arrived_weights = [weights[:, :slots]]
    for m in range(1, owners):
        arrived.append(hop(outgoing[m * slots : (m + 1) * slots], "fs", m))
        arrived_weights.append(hop(weights[:, m * slots : (m + 1) * slots], "fs", m))
    rows = jnp.concatenate(arrived, axis=0)
    row_weights = jnp.concatenate(arrived_weights, axis=1)

    up_pieces, after = send(up_train, True, 0, share_rows, (after, outgoing, weights))
    pieces = [(gate_pieces, 0, share_rows), (up_pieces, 0, share_rows)]
    for first, size in zip(firsts, sizes):
        down_pieces, after = send(down_train, False, first, size, after)
        pieces.append((down_pieces, first, size))

    last = rows
    blocks = []
    for chunk, first, size in pieces:
        chunk_blocks = []
        for piece in chunk:
            piece, _ = lax.optimization_barrier((piece, last))
            last = piece
            chunk_blocks.append([piece] + swap(piece))
        blocks.append(chunk_blocks)

    slots_all = owners * slots
    section = jnp.zeros((splits, slots_all, feats), bf16)
    for m in range(splits):
        block = hop(rows, "tp", m) if m else rows
        section = lax.dynamic_update_slice(
            section, block[None], (origin(split, m, splits), 0, 0)
        )
    squares = jnp.sum(jnp.square(section.astype(f32)), axis=(0, 2))
    row_scale = lax.rsqrt(squares / model_width + 1e-06)

    def product(train, chunk_blocks):
        serve = place(begin(), 0, own(train, True, 0, share_rows), 0)
        for m, parts in zip(range(1, owners), chunk_blocks):
            serve = place(serve, m, parts, 0)
        serve = serve.reshape(per_owner, model_width, hidden_here)
        view = serve.reshape(per_owner, splits, feats, hidden_here)
        total = jnp.einsum("krc,ekcf->erf", section, view, preferred_element_type=f32)
        return serve, row_scale[None, :, None] * total

    gate_serve, gate_pre = product(gate_train, blocks[0])
    gate_act = row_weights[:, :, None] * jax.nn.silu(gate_pre)
    up_serve, up_pre = product(up_train, blocks[1])
    hidden = (gate_act * up_pre).astype(bf16)

    down_serve = begin()
    outs = []
    for (_, first, size), chunk_blocks in zip(pieces[2:], blocks[2:]):
        chunk_blocks = [own(down_train, False, first, size)] + chunk_blocks
        partials = []
        for m, parts in enumerate(chunk_blocks):
            down_serve = place(down_serve, m, parts, first)
            partials.append(
                jnp.stack(
                    [
                        jnp.einsum("edf,erf->dr", part, hidden, preferred_element_type=f32)
                        for part in parts
                    ]
                ).astype(bf16)
            )
        if owners == splits:
            stacked = jnp.stack(partials).reshape(splits, copies * size, slots_all)
            spots = [distance(here, target(split, m, splits), owners) for m in range(splits)]
        else:
            spread = jnp.zeros((owners, copies, size, slots_all), bf16)
            for m, part in enumerate(partials):
                for k in range(copies):
                    spot = (origin(here, m, owners), origin(copy, k, copies), 0, 0)
                    spread = lax.dynamic_update_slice(spread, part[None, k : k + 1], spot)
            stacked = spread.reshape(splits, feats, slots_all)
            spots = [target(split, m, splits) for m in range(splits)]
        total = 0.0
        for m in range(splits):
            block = lax.dynamic_index_in_dim(stacked, spots[m], 0, False)
            block = hop(block, "tp", m) if m else block
            total = total + block.astype(f32)
        total = total.astype(bf16)
        back = [total[:, :slots]]
        for m in range(1, owners):
            back.append(hop_back(total[:, m * slots : (m + 1) * slots], "fs", m))
        back = jnp.concatenate(back, axis=1)
        outs.append(
            lax.dot_general(
                back, pick_rows, (((1,), (1,)), ((), ())), preferred_element_type=f32
            ).astype(bf16)
        )
    if owners == splits:
        outs = [out.reshape(copies, -1, tok_rows) for out in outs]
        out = jnp.concatenate(outs, axis=1)
        out = jnp.stack(
            [
                lax.dynamic_index_in_dim(out, distance(copy, share, copies), 0, False)
                for share in range(copies)
            ]
        )
        moe_out = out.reshape(feats, tok_rows).T
    else:
        moe_out = outs[0].T
    return gate_serve, up_serve, down_serve.reshape(gate_serve.shape), moe_out


def solution(mesh):
    in_specs = (
        P(("grp", "fs"), "tp"),
        P(("grp", "fs"), None),
        P(("grp", "fs")),
        P(("grp", "fs")),
        P(),
        P(None, "fs", "tp"),
        P(None, "fs", "tp"),
        P(None, "fs", "tp"),
    )
    out_specs = (
        P(("grp", "fs"), None, "tp"),
        P(("grp", "fs"), None, "tp"),
        P(("grp", "fs"), None, "tp"),
        P(("grp", "fs"), "tp"),
    )
    return jax.shard_map(shards, mesh=mesh, in_specs=in_specs, out_specs=out_specs, check_vma=False)
```
